32 devices in a mesh: kv: 8 (over z, y), tp: 4 (over x, core).
Axes of the slice: x: 2, y: 2, z: 4, core: 2. Of those that a mesh axis runs over, the one named last changes fastest.
Arguments:
- residual_entries: bfloat16 [512, 4096], P(None, ('kv', 'tp')), may hold values from -6 to 6
- fresh_extents: int32 [64], replicated, may hold values from 1 to 8, 256 in all
- memory_matrix: float32 [64, 16, 128, 128], P('kv', 'tp'), may hold values from -3 to 3
- initial_rescale_vector: float32 [4096], P('kv'), may hold values from 0.1 to 1.9
- probe_matrix: bfloat16 [4096, 2048], P('kv', 'tp'), may hold values from -0.09375 to 0.09375
- retain_matrix: bfloat16 [4096, 2048], P('kv', 'tp'), may hold values from -0.09375 to 0.09375
- content_matrix: bfloat16 [4096, 2048], P('kv', 'tp'), may hold values from -0.09375 to 0.09375
- result_switch_matrix: bfloat16 [4096, 2048], P('kv', 'tp'), may hold values from -0.09375 to 0.09375
- retain_lower_limit: float32 [2048], P('tp'), may hold values from 0 to 0.9
- extra_shrink_log: float32 [512, 16], P('kv', 'tp'), may hold values from -0.7 to 0
- lane_result_rescale: float32 [128], replicated, may hold values from 0.1 to 1.9
- result_matrix: bfloat16 [2048, 4096], P('tp', 'kv'), may hold values from -0.125 to 0.125
- later_rescale_vector: float32 [4096], P(('kv', 'tp')), may hold values from 0.1 to 1.9
- mixer_switch_matrix: bfloat16 [4096, 11008], P(None, ('kv', 'tp')), may hold values from -0.09375 to 0.09375
- widening_matrix: bfloat16 [4096, 11008], P(None, ('kv', 'tp')), may hold values from -0.09375 to 0.09375
- narrowing_matrix: bfloat16 [11008, 4096], P(('kv', 'tp')), may hold values from -0.109375 to 0.109375
Outputs:
- mixed: bfloat16 [512, 4096], P(None, ('kv', 'tp'))
- new_state: float32 [64, 16, 128, 128], P('kv', 'tp')
The draws below stay inside these ranges and needn't reach their ends.
Inputs may be any that keep to these rules, and one draw needn't show every extreme that they name: `fresh_extents`: the lengths sum to exactly 256.
All inputs are finite; a program needn't handle non-finite values.
Results may differ from the reference program's by a relative error of at most 0.022.
Values may be sent and summed in bfloat16 or wider, within the bound.
A program may use at most 64 MiB of HBM per device.

```python
import math
import jax
import jax.numpy as jnp
import numpy as np
from jax import lax

D = 4096
MIXER_LANES = 16
HEAD = 128
FF = 11008
FRESH_PLACES = 8
STRING_TOTAL = 64
PLACE_TOTAL = 512
WIDTH = 2048
N_TP = 4


def with_spikes(result, rng, source, target, parts, factor):
    owner, partner = [(jnp.arange(result.shape[dim]) // (result.shape[dim] // parts)).reshape([-1 if axis == dim else 1 for axis in range(result.ndim)]) for dim in (source, target)]
    chosen = jax.random.permutation(rng, parts)[partner]
    strong = (owner == chosen) | (owner == (partner + parts // 2) % parts)
    return jnp.where(strong, factor * result, result)


def level_of(stream_key, extent, cuts, low, high):
    def one(dim, blocks):
        heights = jax.random.uniform(jax.random.fold_in(jax.random.fold_in(stream_key, 6), dim), (blocks,), jnp.float32, low / len(cuts), high / len(cuts))
        return jnp.repeat(jnp.exp(heights), extent[dim] // blocks).reshape((-1,) + (1,) * (len(extent) - dim - 1))

    level = one(*cuts[0])
    for cut in cuts[1:]:
        level = level * one(*cut)
    return level


def profile(count, total, limit, skew):
    portions = [(1 << 20) // math.isqrt(standing ** skew) + 1 for standing in range(2, count + 1)]
    spare, counts = total - limit - (count - 1), [1] * (count - 1)
    while spare > 0:
        candidates = [i for i in range(count - 1) if counts[i] < limit]
        whole, budget = sum([portions[i] for i in candidates]), spare
        for i in candidates:
            extra = min(limit - counts[i], max(1, budget * portions[i] // whole), spare)
            counts[i] = counts[i] + extra
            spare = spare - extra
    return np.array([limit] + counts)


def uneven(stream_key, number_of, total, most, slope):
    if number_of == 2:
        one = jax.random.randint(stream_key, (), max(1, total - most), min(most, total - 1) + 1)
        return jnp.stack([one, total - one])
    lengths = jnp.asarray(profile(number_of, total, most, slope), jnp.int32)
    twos = (number_of - 1) // 2
    giver, sink = lengths[1:1 + 2 * twos:2], lengths[2:2 + 2 * twos:2]
    slack = jnp.minimum(giver - 1, most - sink)
    shifted = jax.random.randint(jax.random.fold_in(stream_key, 1), (twos,), 0, 1 << 20) % (slack + 1)
    lengths = lengths.at[1:1 + 2 * twos:2].set(giver - shifted).at[2:2 + 2 * twos:2].set(sink + shifted)
    return lengths[jax.random.permutation(jax.random.fold_in(stream_key, 2), number_of)]


def normal_values(key, extent, width, limit, cuts=(), kind=jnp.bfloat16):
    level = level_of(key, extent, cuts, -0.22, 0.18) if cuts else 1.0
    array = jax.random.normal(key, extent, jnp.float32) * width * level
    return jnp.minimum(jnp.maximum(array, -limit), limit).astype(kind)


def bell_draw_with(key, shape, deviation, reach, split, heavy, kind=jnp.bfloat16):
    array = deviation * jax.random.normal(key, shape, jnp.float32)
    if split:
        array = array * level_of(key, shape, split, -0.22, 0.18)
    return jnp.clip(with_spikes(array, jax.random.fold_in(key, 3), *heavy), -reach, reach).astype(kind)


def setup_inputs(seed: int = 0) -> dict:
    key_of = jax.random.split(jax.random.key(seed), 17)
    return {
        "residual_entries": normal_values(key_of[0], (PLACE_TOTAL, D), 1.0, 6.0, ((1, 32),)),
        "fresh_extents": uneven(key_of[1], STRING_TOTAL, STRING_TOTAL * FRESH_PLACES // 2, FRESH_PLACES, 2).astype(jnp.int32),
        "memory_matrix": normal_values(key_of[2], (STRING_TOTAL, MIXER_LANES, HEAD, HEAD), 0.3, 3.0, ((0, 8), (1, 4)), jnp.float32),
        "initial_rescale_vector": jnp.clip(1.0 + 0.18 * jax.random.normal(key_of[3], (D,), jnp.float32), 0.1, 1.9),
        "probe_matrix": normal_values(key_of[4], (D, WIDTH), D ** -0.5, 0.09375, ((0, 8), (1, 4))),
        "retain_matrix": normal_values(key_of[5], (D, WIDTH), D ** -0.5, 0.09375, ((0, 8), (1, 4))),
        "content_matrix": normal_values(key_of[6], (D, WIDTH), D ** -0.5, 0.09375, ((0, 8), (1, 4))),
        "result_switch_matrix": normal_values(key_of[7], (D, WIDTH), D ** -0.5, 0.09375, ((0, 8), (1, 4))),
        "retain_lower_limit": jnp.clip(0.9 * jax.random.uniform(key_of[8], (WIDTH,), jnp.float32) ** level_of(key_of[8], (WIDTH,), ((0, 4),), -0.2, 0.2), 0.0, 0.9),
        "extra_shrink_log": jnp.clip(-0.7 + 0.7 * jax.random.uniform(key_of[9], (PLACE_TOTAL, MIXER_LANES), jnp.float32) ** level_of(key_of[9], (PLACE_TOTAL, MIXER_LANES), ((0, 8), (1, 4)), -0.2, 0.2), -0.7, 0.0),
        "lane_result_rescale": jnp.clip(1.0 + 0.18 * jax.random.normal(key_of[10], (HEAD,), jnp.float32), 0.1, 1.9),
        "result_matrix": normal_values(key_of[11], (WIDTH, D), WIDTH ** -0.5, 0.125, ((0, 4), (1, 8))),
        "later_rescale_vector": jnp.clip(1.0 + 0.18 * jax.random.normal(key_of[12], (D,), jnp.float32), 0.1, 1.9),
        "mixer_switch_matrix": normal_values(key_of[13], (D, FF), D ** -0.5, 0.09375, ((1, 32),)),
        "widening_matrix": normal_values(key_of[14], (D, FF), D ** -0.5, 0.09375, ((1, 32),)),
        "narrowing_matrix": bell_draw_with(key_of[15], (FF, D), FF ** -0.5, 0.109375, ((0, 32),), (0, 1, 32, 2.75)),
    }


epsilon = 1e-06

def reference(residual_entries, fresh_extents, memory_matrix, initial_rescale_vector, probe_matrix, retain_matrix, content_matrix, result_switch_matrix, retain_lower_limit, extra_shrink_log, lane_result_rescale, result_matrix, later_rescale_vector, mixer_switch_matrix, widening_matrix, narrowing_matrix):
    tokens_wide = residual_entries.astype(jnp.float32)
    first_scale = lax.rsqrt(lax.optimization_barrier(jnp.mean(tokens_wide * tokens_wide, axis=1)) + epsilon)
    scaled = (tokens_wide * initial_rescale_vector).astype(jnp.bfloat16)

    def project(weight):
        return jnp.dot(scaled, weight, preferred_element_type=jnp.float32) * first_scale[:, None]
    shape_four = (STRING_TOTAL, FRESH_PLACES, MIXER_LANES, HEAD)
    z_query = project(probe_matrix)
    z_forget = project(retain_matrix).reshape(shape_four)
    z_input = project(content_matrix).reshape(shape_four)
    z_outgate = project(result_switch_matrix)
    living = jnp.arange(FRESH_PLACES, dtype=jnp.int32)[None, :] < fresh_extents[:, None]
    query = jax.nn.silu(z_query).reshape(shape_four)
    bounds = retain_lower_limit.reshape(MIXER_LANES, HEAD)
    retain_factor = bounds + (1.0 - bounds) * jax.nn.sigmoid(z_forget)
    shrink_exponent = jnp.log(retain_factor) + extra_shrink_log.reshape(STRING_TOTAL, FRESH_PLACES, MIXER_LANES, 1)
    decays = jnp.where(living[:, :, None, None], jnp.exp(shrink_exponent), 1.0)
    key_gate = jnp.where(living[:, :, None, None], 1.0 - retain_factor, 0.0)
    carried = memory_matrix
    outputs = []
    for position in range(FRESH_PLACES):
        carried = decays[:, position, :, :, None] * carried + key_gate[:, position, :, :, None] * z_input[:, position, :, None, :]
        outputs.append(jnp.einsum('bhd,bhdv->bhv', query[:, position], carried, precision=lax.Precision.HIGHEST))
    heads_out = jnp.stack(outputs, axis=1)
    heads_out = heads_out * lax.rsqrt(lax.optimization_barrier(jnp.mean(heads_out * heads_out, axis=-1, keepdims=True)) + epsilon) * lane_result_rescale
    live_rows = living.reshape(PLACE_TOTAL)
    normed = jnp.where(live_rows[:, None], heads_out.reshape(PLACE_TOTAL, WIDTH) * jax.nn.silu(z_outgate), 0.0).astype(jnp.bfloat16)
    group_width = WIDTH // N_TP
    attended = jnp.zeros((PLACE_TOTAL, D), jnp.float32)
    for group in range(N_TP):
        head_partial = jnp.dot(normed[:, group * group_width:(group + 1) * group_width], result_matrix[group * group_width:(group + 1) * group_width], preferred_element_type=jnp.float32).astype(jnp.bfloat16)
        attended = attended + head_partial.astype(jnp.float32)
    residual = (tokens_wide + attended).astype(jnp.bfloat16)
    resid_wide = residual.astype(jnp.float32)
    second_scale = lax.rsqrt(lax.optimization_barrier(jnp.mean(resid_wide * resid_wide, axis=1)) + epsilon)
    second_in = (resid_wide * later_rescale_vector * second_scale[:, None]).astype(jnp.bfloat16)
    gated = jnp.dot(second_in, mixer_switch_matrix, preferred_element_type=jnp.float32)
    upward = jnp.dot(second_in, widening_matrix, preferred_element_type=jnp.float32)
    hidden = (jax.nn.silu(gated) * upward).astype(jnp.bfloat16)
    down_terms = jnp.dot(hidden, narrowing_matrix, preferred_element_type=jnp.float32)
    mixed = jnp.where(live_rows[:, None], resid_wide + down_terms, 0.0).astype(jnp.bfloat16)
    return (mixed, carried)
```

```python
import functools

import jax
import jax.numpy as jnp
from jax import lax
from jax.experimental import pallas as pl
from jax.experimental.pallas import tpu as pltpu
from jax.sharding import PartitionSpec as P

FRESH_PLACES = 8
CORES = 2
epsilon = 1e-06

F32, BF16 = jnp.float32, jnp.bfloat16
VM = pl.BlockSpec(memory_space=pltpu.VMEM)
HBM = pl.BlockSpec(memory_space=pl.ANY)
LIMIT = 60 * 1024 * 1024


class Place:
    def __init__(self, kv_size, tp_size):
        self.sizes = {
            "z": 4 if kv_size % 4 == 0 else kv_size,
            "y": kv_size // 4 if kv_size % 4 == 0 else 1,
            "x": tp_size // CORES,
            "c": CORES,
        }
        kv, tp = lax.axis_index("kv"), lax.axis_index("tp")
        width = self.sizes["y"]
        self.at = {"z": kv // width, "y": kv % width, "x": tp // CORES, "c": tp % CORES}

    def partner(self, axis, step):
        return (self.at[axis] + step) % self.sizes[axis]

    def device(self, **moved):
        at = {**self.at, **moved}
        return (at["z"] * self.sizes["y"] + at["y"], at["x"] * CORES + at["c"])


def greet(devices):
    barrier = pltpu.get_barrier_semaphore()
    for device in devices:
        pl.semaphore_signal(
            barrier, inc=1, device_id=device, device_id_type=pl.DeviceIdType.MESH
        )
    pl.semaphore_wait(barrier, len(devices))


def along(place, axes):
    return [
        place.device(**{axis: place.partner(axis, step)})
        for axis in axes
        for step in range(1, place.sizes[axis])
    ]


class Sender:
    def __init__(self, send_sems, recv_sems):
        self.send_sems, self.recv_sems, self.used, self.copies = send_sems, recv_sems, 0, []

    def start(self, source, target, device):
        copy = pltpu.make_async_remote_copy(
            src_ref=source,
            dst_ref=target,
            send_sem=self.send_sems.at[self.used],
            recv_sem=self.recv_sems.at[self.used],
            device_id=device,
            device_id_type=pl.DeviceIdType.MESH,
        )
        self.used += 1
        copy.start()
        self.copies.append(copy)
        return copy

    def finish(self):
        for copy in self.copies:
            copy.wait_send()


def gather_index(place, done):
    return tuple(
        slice(None) if axis in done else place.at[axis] for axis in ("z", "y", "x", "c")
    )


def project_kernel(
    kv_size, tp_size, x_ref, gain_ref, w0, w1, w2, w3, out_ref, sq_ref,
    xg, scaled, part, yrecv, zpart, zrecv, sqpart, sqy, sqz, sqzrecv, send_sems, recv_sems,
):
    place = Place(kv_size, tp_size)
    rows, block = x_ref.shape
    greet(along(place, ("x", "c", "y", "z")))
    sender = Sender(send_sems, recv_sems)
    x, c, y, z = (place.at[axis] for axis in ("x", "c", "y", "z"))
    sizes = place.sizes
    copies = [
        sender.start(x_ref, xg.at[x, c], place.device(x=place.partner("x", step)))
        for step in range(1, sizes["x"])
    ]
    xg[x, c] = x_ref[...]
    for copy in copies:
        copy.wait_recv()
    sender.start(xg.at[:, c], xg.at[:, c], place.device(c=place.partner("c", 1))).wait_recv()
    squares = jnp.zeros((rows, block), F32)
    for t in range(tp_size):
        wide = xg[t // CORES, t % CORES].astype(F32)
        squares += wide * wide
        lanes = slice(t * block, (t + 1) * block)
        scaled[:, lanes] = (wide * gain_ref[:, lanes]).astype(BF16)
    sqpart[...] = squares.astype(BF16).reshape(sqpart.shape)

    def y_stage(source, landing):
        return [
            sender.start(
                source.at[:, place.partner("y", step)],
                landing.at[step - 1],
                place.device(y=place.partner("y", step)),
            )
            for step in range(1, sizes["y"])
        ]

    def y_sum(copies, source, landing):
        for copy in copies:
            copy.wait_recv()
        total = source[:, y].astype(F32)
        for step in range(1, sizes["y"]):
            total += landing[step - 1].astype(F32)
        return total.astype(BF16)

    def z_stage(source, landing):
        return [
            sender.start(
                source.at[place.partner("z", step)],
                landing.at[step - 1],
                place.device(z=place.partner("z", step)),
            )
            for step in range(1, sizes["z"])
        ]

    def z_sum(copies, source, landing):
        for copy in copies:
            copy.wait_recv()
        total = source[z].astype(F32)
        for step in range(1, sizes["z"]):
            total += landing[step - 1].astype(F32)
        return total

    in_y = [y_stage(sqpart, sqy)]
    for m, w in enumerate((w0, w1, w2, w3)):
        product = jnp.dot(scaled[...], w[...], preferred_element_type=F32)
        part[m] = product.astype(BF16).reshape(part.shape[1:])
        in_y.append(y_stage(part.at[m], yrecv.at[m]))
    sqz[...] = y_sum(in_y[0], sqpart, sqy)
    in_z = [z_stage(sqz, sqzrecv)]
    for m in range(4):
        zpart[m] = y_sum(in_y[m + 1], part.at[m], yrecv.at[m])
        in_z.append(z_stage(zpart.at[m], zrecv.at[m]))
    sq_ref[...] = z_sum(in_z[0], sqz, sqzrecv)
    for m in range(4):
        out_ref[m] = z_sum(in_z[m + 1], zpart.at[m], zrecv.at[m])
    sender.finish()


def recur_kernel(
    features, z_ref, sq_ref, state_ref, low_ref, shrink_ref, live_ref, lane_ref,
    normed_ref, new_ref,
):
    sequences, heads, head, _ = state_ref.shape
    rows = sequences * FRESH_PLACES
    scale = lax.rsqrt(jnp.sum(sq_ref[...], axis=1, keepdims=True) / features + epsilon)
    live = live_ref[...] > 0.5
    slot = lax.broadcasted_iota(jnp.int32, (rows, head), 0) % FRESH_PLACES
    owner = lax.broadcasted_iota(jnp.int32, (rows, head), 0) // FRESH_PLACES

    def back(value, step, fill):
        if step == 0:
            return value
        return jnp.where(slot >= step, pltpu.roll(value, step, 0), fill)

    def ahead(value, step, fill):
        return jnp.where(slot < FRESH_PLACES - step, pltpu.roll(value, rows - step, 0), fill)

    for h in range(heads):
        lanes = slice(h * head, (h + 1) * head)
        zq, zf, v, zg = (z_ref[m, :, lanes] * scale for m in range(4))
        query = zq * jax.nn.sigmoid(zq)
        low = low_ref[:, lanes]
        forget = low + (1.0 - low) * jax.nn.sigmoid(zf)
        decay = jnp.where(live, jnp.exp(jnp.log(forget) + shrink_ref[:, lanes]), 1.0)
        key = jnp.where(live, 1.0 - forget, 0.0)
        prefix, suffix = decay, ahead(decay, 1, 1.0)
        for step in (1, 2, 4):
            prefix = prefix * back(prefix, step, 1.0)
            suffix = suffix * ahead(suffix, step, 1.0)
        out = jnp.sum(query * key, axis=1, keepdims=True) * v
        weight = query
        for step in range(1, FRESH_PLACES):
            weight = weight * back(decay, step - 1, 0.0)
            near = jnp.sum(weight * back(key, step, 0.0), axis=1, keepdims=True)
            out += near * back(v, step, 0.0)
        reach = (query * prefix).astype(BF16)
        key_t = (key * suffix).T.astype(BF16)
        prefix_t = prefix.T
        v16 = v.astype(BF16)
        old = []
        for s in range(sequences):
            mine = slice(s * FRESH_PLACES, (s + 1) * FRESH_PLACES)
            before = state_ref[s, h]
            old.append(
                jnp.dot(reach[mine], before.astype(BF16), preferred_element_type=F32)
            )
            last = (s + 1) * FRESH_PLACES - 1
            added = jnp.dot(
                key_t, jnp.where(owner == s, v, 0.0).astype(BF16), preferred_element_type=F32
            )
            new_ref[s, h] = prefix_t[:, last : last + 1] * before + added
        out += jnp.concatenate(old, axis=0)
        out = out * lax.rsqrt(jnp.mean(out * out, axis=1, keepdims=True) + epsilon)
        out = out * lane_ref[...] * (zg * jax.nn.sigmoid(zg))
        normed_ref[:, lanes] = jnp.where(live, out, 0.0).astype(BF16)


def attend_kernel(
    kv_size, tp_size, n_ref, pick_ref, w_ref, x_ref, resid_ref,
    ng, heads_part, landed, send_sems, recv_sems,
):
    place = Place(kv_size, tp_size)
    sizes = place.sizes
    z, y, x, c = (place.at[axis] for axis in ("z", "y", "x", "c"))
    steps = [(i, j) for i in range(sizes["x"]) for j in range(CORES) if i or j]
    across = [
        (place.partner("x", i), place.partner("c", j)) for i, j in steps
    ]
    greet(along(place, ("z", "y")) + [place.device(x=i, c=j) for i, j in across])
    sender = Sender(send_sems, recv_sems)
    copies = [
        sender.start(n_ref, ng.at[z, y], place.device(z=place.partner("z", step)))
        for step in range(1, sizes["z"])
    ]
    ng[z, y] = n_ref[...]
    for copy in copies:
        copy.wait_recv()
    copies = [
        sender.start(ng.at[:, y], ng.at[:, y], place.device(y=place.partner("y", step)))
        for step in range(1, sizes["y"])
    ]
    pick = pick_ref[...]
    own = jnp.dot(pick, x_ref[...], preferred_element_type=F32)
    for copy in copies:
        copy.wait_recv()
    every = ng[...].reshape(pick.shape[1], n_ref.shape[1])
    chosen = jnp.dot(pick, every, preferred_element_type=F32).astype(BF16)
    product = jnp.dot(chosen, w_ref[...], preferred_element_type=F32).astype(BF16)
    block = x_ref.shape[1]
    for t in range(tp_size):
        heads_part[t] = product[:, t * block : (t + 1) * block]
    copies = [
        sender.start(heads_part.at[i * CORES + j], landed.at[n], place.device(x=i, c=j))
        for n, (i, j) in enumerate(across)
    ]
    total = heads_part[x * CORES + c].astype(F32)
    for n, copy in enumerate(copies):
        copy.wait_recv()
        total += landed[n].astype(F32)
    resid_ref[...] = (own + total).astype(BF16)
    sender.finish()


def mixer_kernel(
    kv_size, tp_size, x_ref, gain_ref, wg_hbm, wu_hbm, wd_hbm, out_ref,
    xg, gg, wg, wu, wd, own_part, core_part, core_recv, recvs, parts,
    send_sems, recv_sems, load_sems,
):
    place = Place(kv_size, tp_size)
    sizes = place.sizes
    at = place.at
    rows, block = x_ref.shape
    half = rows // 2
    features = kv_size * tp_size * block
    loads = [
        pltpu.make_async_copy(source, target, load_sems.at[n])
        for n, (source, target) in enumerate(((wg_hbm, wg), (wu_hbm, wu), (wd_hbm, wd)))
    ]
    for load in loads:
        load.start()
    greet(along(place, ("z", "y", "x", "c")))
    sender = Sender(send_sems, recv_sems)

    orders = (("z", "y", "x", "c"), ("z", "x", "y", "c"))

    def view(ref, done, span):
        lead = tuple(slice(None) if axis in done else at[axis] for axis in ("z", "y", "x"))
        if "c" in done:
            return ref.at[lead + (span, slice(None))]
        return ref.at[lead + (span, pl.ds(pl.multiple_of(at["c"] * block, block), block))]

    spans = [pl.ds(0, half), pl.ds(half, half)]

    def push(h, level):
        axis, done = orders[h][level], orders[h][:level]
        started = []
        for step in range(1, sizes[axis]):
            device = place.device(**{axis: place.partner(axis, step)})
            target = view(xg, done, spans[h])
            source = x_ref.at[spans[h]] if level == 0 else target
            started.append(sender.start(source, target, device))
            if h == 0:
                target = view(gg, done, slice(None))
                started.append(sender.start(gain_ref if level == 0 else target, target, device))
        return started

    flying = [push(0, 0), push(1, 0)]
    mine = pl.ds(pl.multiple_of(at["c"] * block, block), block)
    xg[at["z"], at["y"], at["x"], :, mine] = x_ref[...]
    gg[at["z"], at["y"], at["x"], :, mine] = gain_ref[...]
    for level in range(1, 5):
        for h in range(2):
            for copy in flying[h]:
                copy.wait_recv()
            if level < 4:
                flying[h] = push(h, level)
    for load in loads:
        load.wait()

    units = [
        (i, j, k)
        for i in range(sizes["z"])
        for j in range(sizes["y"])
        for k in range(sizes["x"])
    ]
    wide = CORES * block
    hidden_units = wg.shape[1]
    gated = jnp.zeros((rows, hidden_units), F32)
    upward = jnp.zeros((rows, hidden_units), F32)
    squares = jnp.zeros((rows, wide), F32)
    for n, unit in enumerate(units):
        value = xg[unit].astype(F32)
        squares += value * value
        piece = (value * gg[unit][:1]).astype(BF16)
        gated += jnp.dot(piece, wg[n * wide : (n + 1) * wide], preferred_element_type=F32)
        upward += jnp.dot(piece, wu[n * wide : (n + 1) * wide], preferred_element_type=F32)
    scale = lax.rsqrt(jnp.sum(squares, axis=1, keepdims=True) / features + epsilon)
    gated, upward = gated * scale, upward * scale
    hidden = (gated * jax.nn.sigmoid(gated) * upward).astype(BF16)

    copies = []
    for n, unit in enumerate(units):
        product = jnp.dot(hidden, wd[:, n * wide : (n + 1) * wide], preferred_element_type=F32)
        low, high = product[:, :block], product[:, block:]
        first = at["c"] == 0
        own_part[unit] = jnp.where(first, low, high)
        core_part[unit] = jnp.where(first, high, low).astype(BF16)
        if unit[1:] == (sizes["y"] - 1, sizes["x"] - 1):
            copies.append(
                sender.start(
                    core_part.at[unit[0]], core_recv.at[unit[0]],
                    place.device(c=place.partner("c", 1)),
                )
            )
    for copy in copies:
        copy.wait_recv()
    sums = (("x", "y", "z"), ("y", "x", "z"))
    axes = ("z", "y", "x")

    def index(h, done, moved=None):
        picked = []
        for axis in axes:
            if moved is not None and axis == moved[0]:
                picked.append(moved[1])
            elif axis in done:
                picked.append(at[axis])
            else:
                picked.append(slice(None))
        return tuple(picked)

    def add_core(h):
        span = slice(h * half, (h + 1) * half)
        return own_part[:, :, :, span] + core_recv[:, :, :, span].astype(F32)

    def send(h, level):
        axis, done = sums[h][level], sums[h][:level]
        source = parts[h][level]
        keep = [a for a in axes if a not in done]
        started = []
        for step in range(1, sizes[axis]):
            other = place.partner(axis, step)
            where = tuple(other if a == axis else slice(None) for a in keep)
            started.append(
                sender.start(
                    source.at[where] if where else source,
                    recvs[h][level].at[step - 1],
                    place.device(**{axis: other}),
                )
            )
        return started

    def reduce(h, level, copies):
        axis, done = sums[h][level], sums[h][:level]
        keep = [a for a in axes if a not in done]
        where = tuple(at[a] if a == axis else slice(None) for a in keep)
        for copy in copies:
            copy.wait_recv()
        total = parts[h][level][where].astype(F32)
        for step in range(1, sizes[axis]):
            total += recvs[h][level][step - 1].astype(F32)
        return total

    flying = []
    for h in range(2):
        parts[h][0][...] = add_core(h).astype(BF16)
        flying.append(send(h, 0))
    for level in range(2):
        for h in range(2):
            parts[h][level + 1][...] = reduce(h, level, flying[h]).astype(BF16)
            flying[h] = send(h, level + 1)
    for h in range(2):
        span = slice(h * half, (h + 1) * half)
        down = reduce(h, 2, flying[h])
        out_ref[span] = (x_ref[span].astype(F32) + down).astype(BF16)
    sender.finish()


def remote(kernel, out_shape, specs, scratch, name, identity):
    return pl.pallas_call(
        kernel,
        out_shape=out_shape,
        in_specs=specs,
        out_specs=jax.tree.map(lambda _: VM, out_shape),
        scratch_shapes=scratch,
        compiler_params=pltpu.CompilerParams(
            collective_id=identity, has_side_effects=True, vmem_limit_bytes=LIMIT
        ),
        name=name,
    )


def local(
    kv_size,
    tp_size,
    residual_entries,
    fresh_extents,
    memory_matrix,
    initial_rescale_vector,
    probe_matrix,
    retain_matrix,
    content_matrix,
    result_switch_matrix,
    retain_lower_limit,
    extra_shrink_log,
    lane_result_rescale,
    result_matrix,
    later_rescale_vector,
    mixer_switch_matrix,
    widening_matrix,
    narrowing_matrix,
):
    sequences, heads, head, _ = memory_matrix.shape
    own_rows = sequences * FRESH_PLACES
    all_rows, block = residual_entries.shape
    live_count = all_rows // 2
    width = probe_matrix.shape[1]
    features = block * kv_size * tp_size
    kv_index = lax.axis_index("kv")
    nz = 4 if kv_size % 4 == 0 else kv_size
    ny, nx = kv_size // nz, tp_size // CORES
    dma = pltpu.SemaphoreType.DMA

    strings = fresh_extents.shape[0]
    earlier = jnp.arange(strings)[:, None] < jnp.arange(strings)[None, :]
    starts = jnp.sum(jnp.where(earlier, fresh_extents[:, None], 0), axis=0)
    places = jnp.arange(FRESH_PLACES, dtype=jnp.int32)[None, :]
    living = places < fresh_extents[:, None]
    rank = jnp.where(living, starts[:, None] + places, -1).reshape(1, all_rows)
    pick = (rank == jnp.arange(live_count, dtype=jnp.int32)[:, None]).astype(BF16)

    count = (nx - 1) + 1 + 5 * (ny - 1 + nz - 1)
    projected, squares = remote(
        functools.partial(project_kernel, kv_size, tp_size),
        (
            jax.ShapeDtypeStruct((4, own_rows, width), F32),
            jax.ShapeDtypeStruct((own_rows, block), F32),
        ),
        [VM] * 6,
        [
            pltpu.VMEM((nx, CORES, all_rows, block), BF16),
            pltpu.VMEM((all_rows, tp_size * block), BF16),
            pltpu.VMEM((4, nz, ny, own_rows, width), BF16),
            pltpu.VMEM((4, max(ny - 1, 1), nz, own_rows, width), BF16),
            pltpu.VMEM((4, nz, own_rows, width), BF16),
            pltpu.VMEM((4, max(nz - 1, 1), own_rows, width), BF16),
            pltpu.VMEM((nz, ny, own_rows, block), BF16),
            pltpu.VMEM((max(ny - 1, 1), nz, own_rows, block), BF16),
            pltpu.VMEM((nz, own_rows, block), BF16),
            pltpu.VMEM((max(nz - 1, 1), own_rows, block), BF16),
            dma((count,)),
            dma((count,)),
        ],
        "project",
        1,
    )(
        residual_entries,
        initial_rescale_vector.reshape(1, -1),
        probe_matrix,
        retain_matrix,
        content_matrix,
        result_switch_matrix,
    )

    own_living = lax.dynamic_slice_in_dim(living, kv_index * sequences, sequences)
    live = jnp.broadcast_to(own_living.reshape(own_rows, 1), (own_rows, head)).astype(F32)
    shrink = jnp.repeat(extra_shrink_log, head, axis=1)
    normed, new_state = pl.pallas_call(
        functools.partial(recur_kernel, features),
        out_shape=(
            jax.ShapeDtypeStruct((own_rows, width), BF16),
            jax.ShapeDtypeStruct(memory_matrix.shape, F32),
        ),
        in_specs=[VM] * 7,
        out_specs=(VM, VM),
        compiler_params=pltpu.CompilerParams(vmem_limit_bytes=LIMIT),
        name="recur",
    )(
        projected,
        squares,
        memory_matrix,
        retain_lower_limit.reshape(1, -1),
        shrink,
        live,
        lane_result_rescale.reshape(1, -1),
    )

    count = (nz - 1) + (ny - 1) + (tp_size - 1)
    residual = remote(
        functools.partial(attend_kernel, kv_size, tp_size),
        jax.ShapeDtypeStruct((live_count, block), BF16),
        [VM] * 4,
        [
            pltpu.VMEM((nz, ny, own_rows, width), BF16),
            pltpu.VMEM((tp_size, live_count, block), BF16),
            pltpu.VMEM((tp_size - 1, live_count, block), BF16),
            dma((count,)),
            dma((count,)),
        ],
        "attend",
        2,
    )(normed, pick, result_matrix, residual_entries)

    half = live_count // 2
    sizes = {"z": nz, "y": ny, "x": nx}

    def buffers(order):
        left, landing, kept = ["z", "y", "x"], [], []
        for axis in order:
            kept.append(pltpu.VMEM(tuple(sizes[a] for a in left) + (half, block), BF16))
            left = [a for a in left if a != axis]
            landing.append(
                pltpu.VMEM(
                    (max(sizes[axis] - 1, 1),) + tuple(sizes[a] for a in left) + (half, block),
                    BF16,
                )
            )
        return kept, landing

    first, second = buffers(("x", "y", "z")), buffers(("y", "x", "z"))
    hops = nz + ny + nx - 3
    count = 3 * (hops + 1) + nz + 2 * hops
    hidden_units = mixer_switch_matrix.shape[1]
    mixed_live = remote(
        functools.partial(mixer_kernel, kv_size, tp_size),
        jax.ShapeDtypeStruct((live_count, block), BF16),
        [VM, VM, HBM, HBM, HBM],
        [
            pltpu.VMEM((nz, ny, nx, live_count, CORES * block), BF16),
            pltpu.VMEM((nz, ny, nx, 8, CORES * block), F32),
            pltpu.VMEM((features, hidden_units), BF16),
            pltpu.VMEM((features, hidden_units), BF16),
            pltpu.VMEM((hidden_units, features), BF16),
            pltpu.VMEM((nz, ny, nx, live_count, block), F32),
            pltpu.VMEM((nz, ny, nx, live_count, block), BF16),
            pltpu.VMEM((nz, ny, nx, live_count, block), BF16),
            [first[1], second[1]],
            [first[0], second[0]],
            dma((count,)),
            dma((count,)),
            dma((3,)),
        ],
        "mixer",
        3,
    )(
        residual,
        jnp.broadcast_to(later_rescale_vector.reshape(1, -1), (8, block)),
        mixer_switch_matrix,
        widening_matrix,
        narrowing_matrix,
    )
    mixed = jnp.dot(pick.T, mixed_live, preferred_element_type=F32).astype(BF16)
    return (mixed, new_state)


def plain_local(
    residual_entries,
    fresh_extents,
    memory_matrix,
    initial_rescale_vector,
    probe_matrix,
    retain_matrix,
    content_matrix,
    result_switch_matrix,
    retain_lower_limit,
    extra_shrink_log,
    lane_result_rescale,
    result_matrix,
    later_rescale_vector,
    mixer_switch_matrix,
    widening_matrix,
    narrowing_matrix,
):
    sequences_per_device = memory_matrix.shape[0]
    heads_per_device = memory_matrix.shape[1]
    rows_dev = sequences_per_device * FRESH_PLACES
    all_rows = residual_entries.shape[0]
    features = initial_rescale_vector.shape[0] * lax.axis_size("kv")
    kv_index = lax.axis_index("kv")
    tokens_wide = residual_entries.astype(jnp.float32)
    columns = lax.all_gather(residual_entries, "tp", axis=1, tiled=True)
    squares = lax.psum(jnp.sum(tokens_wide * tokens_wide, axis=1), ("kv", "tp"))
    own_squares = lax.dynamic_slice_in_dim(squares, kv_index * rows_dev, rows_dev)
    first_scale = lax.rsqrt(own_squares / features + epsilon)
    scaled = (columns.astype(jnp.float32) * initial_rescale_vector).astype(jnp.bfloat16)
    projected = (
        lax.psum_scatter(
            jnp.concatenate(
                [
                    jnp.dot(scaled, weight, preferred_element_type=jnp.float32)
                    for weight in (
                        probe_matrix,
                        retain_matrix,
                        content_matrix,
                        result_switch_matrix,
                    )
                ],
                axis=1,
            ).astype(jnp.bfloat16),
            "kv",
            scatter_dimension=0,
            tiled=True,
        ).astype(jnp.float32)
        * first_scale[:, None]
    )
    width_dev = probe_matrix.shape[1]
    shape_four = (sequences_per_device, FRESH_PLACES, heads_per_device, memory_matrix.shape[2])
    z_query = projected[:, :width_dev]
    z_forget = projected[:, width_dev : 2 * width_dev].reshape(shape_four)
    z_input = projected[:, 2 * width_dev : 3 * width_dev].reshape(shape_four)
    z_outgate = projected[:, 3 * width_dev :]
    own_lengths = lax.dynamic_slice_in_dim(
        fresh_extents, kv_index * sequences_per_device, sequences_per_device
    )
    living = jnp.arange(FRESH_PLACES, dtype=jnp.int32)[None, :] < own_lengths[:, None]
    query = jax.nn.silu(z_query).reshape(shape_four)
    bounds = retain_lower_limit.reshape(heads_per_device, memory_matrix.shape[2])
    retain_factor = bounds + (1.0 - bounds) * jax.nn.sigmoid(z_forget)
    shrink_exponent = jnp.log(retain_factor) + extra_shrink_log.reshape(
        sequences_per_device, FRESH_PLACES, heads_per_device, 1
    )
    decays = jnp.where(living[:, :, None, None], jnp.exp(shrink_exponent), 1.0)
    key_gate = jnp.where(living[:, :, None, None], 1.0 - retain_factor, 0.0)
    carried = memory_matrix
    outputs = []
    for position in range(FRESH_PLACES):
        carried = (
            decays[:, position, :, :, None] * carried
            + key_gate[:, position, :, :, None] * z_input[:, position, :, None, :]
        )
        outputs.append(
            jnp.einsum(
                "bhd,bhdv->bhv", query[:, position], carried, precision=lax.Precision.HIGHEST
            )
        )
    heads_out = jnp.stack(outputs, axis=1)
    heads_out = (
        heads_out
        * lax.rsqrt(jnp.mean(heads_out * heads_out, axis=-1, keepdims=True) + epsilon)
        * lane_result_rescale
    )
    normed = jnp.where(
        living.reshape(rows_dev)[:, None],
        heads_out.reshape(rows_dev, width_dev) * jax.nn.silu(z_outgate),
        0.0,
    ).astype(jnp.bfloat16)
    head_partial = jnp.dot(
        lax.all_gather(normed, "kv", axis=0, tiled=True),
        result_matrix,
        preferred_element_type=jnp.float32,
    ).astype(jnp.bfloat16)
    attended = lax.psum_scatter(head_partial, "tp", scatter_dimension=1, tiled=True).astype(
        jnp.float32
    )
    residual = (tokens_wide + attended).astype(jnp.bfloat16)
    resid_wide = residual.astype(jnp.float32)
    resid_squares = lax.psum(jnp.sum(resid_wide * resid_wide, axis=1), ("kv", "tp"))
    second_in = (
        resid_wide * later_rescale_vector * lax.rsqrt(resid_squares / features + epsilon)[:, None]
    ).astype(jnp.bfloat16)
    live_rows = (
        jnp.arange(FRESH_PLACES, dtype=jnp.int32)[None, :] < fresh_extents[:, None]
    ).reshape(all_rows)
    live_order = jnp.argsort(1 - live_rows.astype(jnp.int32), stable=True)[: all_rows // 2]
    mixer_input = jnp.take(second_in, live_order, axis=0)
    piece = lax.all_gather(mixer_input, ("kv", "tp"), axis=1, tiled=True)
    gated = jnp.dot(piece, mixer_switch_matrix, preferred_element_type=jnp.float32)
    upward = jnp.dot(piece, widening_matrix, preferred_element_type=jnp.float32)
    hidden = (jax.nn.silu(gated) * upward).astype(jnp.bfloat16)
    mixer_terms = lax.psum_scatter(
        jnp.dot(hidden, narrowing_matrix, preferred_element_type=jnp.float32),
        ("kv", "tp"),
        scatter_dimension=1,
        tiled=True,
    )
    down_terms = (
        jnp.zeros((all_rows, mixer_terms.shape[1]), jnp.float32).at[live_order].set(mixer_terms)
    )
    mixed = jnp.where(live_rows[:, None], resid_wide + down_terms, 0.0).astype(jnp.bfloat16)
    return (mixed, carried)


def solution(mesh):
    placed = (
        P(None, ("kv", "tp")),
        P(),
        P("kv", "tp", None, None),
        P("kv"),
        P("kv", "tp"),
        P("kv", "tp"),
        P("kv", "tp"),
        P("kv", "tp"),
        P("tp"),
        P("kv", "tp"),
        P(),
        P("tp", "kv"),
        P(("kv", "tp")),
        P(None, ("kv", "tp")),
        P(None, ("kv", "tp")),
        P(("kv", "tp"), None),
    )

    def step(residual_entries, *others):
        sizes = mesh.shape["kv"], mesh.shape["tp"]
        if residual_entries.shape[1] % 128:
            return plain_local(residual_entries, *others)
        return local(*sizes, residual_entries, *others)

    return jax.shard_map(
        step,
        mesh=mesh,
        in_specs=placed,
        out_specs=(P(None, ("kv", "tp")), P("kv", "tp", None, None)),
        check_vma=False,
    )
```

```python
import functools

import jax
import jax.numpy as jnp
from jax import lax
from jax.experimental import pallas as pl
from jax.experimental.pallas import tpu as pltpu
from jax.sharding import PartitionSpec as P

FRESH_PLACES = 8
CORES = 2
PIECES = 8
epsilon = 1e-06

F32, BF16 = jnp.float32, jnp.bfloat16
VM = pl.BlockSpec(memory_space=pltpu.VMEM)
HBM = pl.BlockSpec(memory_space=pl.ANY)
LIMIT = 60 * 1024 * 1024


class Place:
    def __init__(self, kv_size, tp_size):
        self.sizes = {
            "z": 4 if kv_size % 4 == 0 else kv_size,
            "y": kv_size // 4 if kv_size % 4 == 0 else 1,
            "x": tp_size // CORES,
            "c": CORES,
        }
        kv, tp = lax.axis_index("kv"), lax.axis_index("tp")
        width = self.sizes["y"]
        self.at = {"z": kv // width, "y": kv % width, "x": tp // CORES, "c": tp % CORES}

    def partner(self, axis, step):
        return (self.at[axis] + step) % self.sizes[axis]

    def device(self, **moved):
        at = {**self.at, **moved}
        return (at["z"] * self.sizes["y"] + at["y"], at["x"] * CORES + at["c"])


def greet(devices):
    barrier = pltpu.get_barrier_semaphore()
    for device in devices:
        pl.semaphore_signal(
            barrier, inc=1, device_id=device, device_id_type=pl.DeviceIdType.MESH
        )
    pl.semaphore_wait(barrier, len(devices))


def along(place, axes):
    return [
        place.device(**{axis: place.partner(axis, step)})
        for axis in axes
        for step in range(1, place.sizes[axis])
    ]


class Sender:
    def __init__(self, send_sems, recv_sems):
        self.send_sems, self.recv_sems, self.used, self.copies = send_sems, recv_sems, 0, []

    def start(self, source, target, device):
        copy = pltpu.make_async_remote_copy(
            src_ref=source,
            dst_ref=target,
            send_sem=self.send_sems.at[self.used],
            recv_sem=self.recv_sems.at[self.used],
            device_id=device,
            device_id_type=pl.DeviceIdType.MESH,
        )
        self.used += 1
        copy.start()
        self.copies.append(copy)
        return copy

    def finish(self):
        for copy in self.copies:
            copy.wait_send()


def gather_index(place, done):
    return tuple(
        slice(None) if axis in done else place.at[axis] for axis in ("z", "y", "x", "c")
    )


def project_kernel(
    kv_size, tp_size, x_ref, gain_ref, w0, w1, w2, w3, out_ref, sq_ref,
    xg, scaled, part, yrecv, zpart, zrecv, sqpart, sqy, sqz, sqzrecv, send_sems, recv_sems,
):
    place = Place(kv_size, tp_size)
    rows, block = x_ref.shape
    greet(along(place, ("x", "c", "y", "z")))
    sender = Sender(send_sems, recv_sems)
    x, c, y, z = (place.at[axis] for axis in ("x", "c", "y", "z"))
    sizes = place.sizes
    copies = [
        sender.start(x_ref, xg.at[x, c], place.device(x=place.partner("x", step)))
        for step in range(1, sizes["x"])
    ]
    xg[x, c] = x_ref[...]
    for copy in copies:
        copy.wait_recv()
    sender.start(xg.at[:, c], xg.at[:, c], place.device(c=place.partner("c", 1))).wait_recv()
    squares = jnp.zeros((rows, block), F32)
    for t in range(tp_size):
        wide = xg[t // CORES, t % CORES].astype(F32)
        squares += wide * wide
        lanes = slice(t * block, (t + 1) * block)
        scaled[:, lanes] = (wide * gain_ref[:, lanes]).astype(BF16)
    sqpart[...] = squares.astype(BF16).reshape(sqpart.shape)

    def y_stage(source, landing):
        return [
            sender.start(
                source.at[:, place.partner("y", step)],
                landing.at[step - 1],
                place.device(y=place.partner("y", step)),
            )
            for step in range(1, sizes["y"])
        ]

    def y_sum(copies, source, landing):
        for copy in copies:
            copy.wait_recv()
        total = source[:, y].astype(F32)
        for step in range(1, sizes["y"]):
            total += landing[step - 1].astype(F32)
        return total.astype(BF16)

    def z_stage(source, landing):
        return [
            sender.start(
                source.at[place.partner("z", step)],
                landing.at[step - 1],
                place.device(z=place.partner("z", step)),
            )
            for step in range(1, sizes["z"])
        ]

    def z_sum(copies, source, landing):
        for copy in copies:
            copy.wait_recv()
        total = source[z].astype(F32)
        for step in range(1, sizes["z"]):
            total += landing[step - 1].astype(F32)
        return total

    in_y = [y_stage(sqpart, sqy)]
    chunk = part.shape[-1]
    for m in range(PIECES):
        w, lanes = (w0, w1, w2, w3)[m // 2], slice(m % 2 * chunk, (m % 2 + 1) * chunk)
        product = jnp.dot(scaled[...], w[:, lanes], preferred_element_type=F32)
        part[m] = product.astype(BF16).reshape(part.shape[1:])
        in_y.append(y_stage(part.at[m], yrecv.at[m]))
    sqz[...] = y_sum(in_y[0], sqpart, sqy)
    in_z = [z_stage(sqz, sqzrecv)]
    for m in range(PIECES):
        zpart[m] = y_sum(in_y[m + 1], part.at[m], yrecv.at[m])
        in_z.append(z_stage(zpart.at[m], zrecv.at[m]))
    sq_ref[...] = z_sum(in_z[0], sqz, sqzrecv)
    for m in range(PIECES):
        out_ref[m // 2, :, m % 2 * chunk : (m % 2 + 1) * chunk] = z_sum(in_z[m + 1], zpart.at[m], zrecv.at[m])
    sender.finish()


def recur_kernel(
    features, z_ref, sq_ref, state_ref, low_ref, shrink_ref, extent_ref, lane_ref, gain_ref,
    normed_ref, new_ref, gain_rows_ref,
):
    sequences, heads, head, _ = state_ref.shape
    rows = sequences * FRESH_PLACES
    scale = lax.rsqrt(jnp.sum(sq_ref[...], axis=1, keepdims=True) / features + epsilon)
    gain_rows_ref[...] = jnp.broadcast_to(gain_ref[...], gain_rows_ref.shape)
    strings = extent_ref.shape[1]
    string = lax.broadcasted_iota(jnp.int32, (rows, strings), 1)
    row = lax.broadcasted_iota(jnp.int32, (rows, strings), 0)
    first = lax.axis_index("kv") * sequences
    extent = jnp.sum(
        jnp.where(string == first + row // FRESH_PLACES, extent_ref[...].astype(F32), 0.0),
        axis=1, keepdims=True,
    )
    slot = lax.broadcasted_iota(jnp.int32, (rows, head), 0) % FRESH_PLACES
    owner = lax.broadcasted_iota(jnp.int32, (rows, head), 0) // FRESH_PLACES

    live = slot.astype(F32) < extent

    def back(value, step, fill):
        if step == 0:
            return value
        return jnp.where(slot >= step, pltpu.roll(value, step, 0), fill)

    def ahead(value, step, fill):
        return jnp.where(slot < FRESH_PLACES - step, pltpu.roll(value, rows - step, 0), fill)

    for h in range(heads):
        lanes = slice(h * head, (h + 1) * head)
        zq, zf, v, zg = (z_ref[m, :, lanes] * scale for m in range(4))
        query = zq * jax.nn.sigmoid(zq)
        low = low_ref[:, lanes]
        forget = low + (1.0 - low) * jax.nn.sigmoid(zf)
        decay = jnp.where(live, jnp.exp(jnp.log(forget) + shrink_ref[:, h : h + 1]), 1.0)
        key = jnp.where(live, 1.0 - forget, 0.0)
        prefix, suffix = decay, ahead(decay, 1, 1.0)
        for step in (1, 2, 4):
            prefix = prefix * back(prefix, step, 1.0)
            suffix = suffix * ahead(suffix, step, 1.0)
        out = jnp.sum(query * key, axis=1, keepdims=True) * v
        weight = query
        for step in range(1, FRESH_PLACES):
            weight = weight * back(decay, step - 1, 0.0)
            near = jnp.sum(weight * back(key, step, 0.0), axis=1, keepdims=True)
            out += near * back(v, step, 0.0)
        reach = (query * prefix).astype(BF16)
        key_t = (key * suffix).T.astype(BF16)
        prefix_t = prefix.T
        v16 = v.astype(BF16)
        old = []
        for s in range(sequences):
            mine = slice(s * FRESH_PLACES, (s + 1) * FRESH_PLACES)
            before = state_ref[s, h]
            old.append(
                jnp.dot(reach[mine], before.astype(BF16), preferred_element_type=F32)
            )
            last = (s + 1) * FRESH_PLACES - 1
            added = jnp.dot(
                key_t, jnp.where(owner == s, v, 0.0).astype(BF16), preferred_element_type=F32
            )
            new_ref[s, h] = prefix_t[:, last : last + 1] * before + added
        out += jnp.concatenate(old, axis=0)
        out = out * lax.rsqrt(jnp.mean(out * out, axis=1, keepdims=True) + epsilon)
        out = out * lane_ref[...] * (zg * jax.nn.sigmoid(zg))
        normed_ref[:, lanes] = jnp.where(live, out, 0.0).astype(BF16)


def pick_rows(extent_ref, count, total):
    strings = extent_ref.shape[1]
    extents = jnp.broadcast_to(extent_ref[...].astype(F32), (16, strings)).astype(BF16)
    string = lax.broadcasted_iota(jnp.int32, (strings, total), 0)
    owner = lax.broadcasted_iota(jnp.int32, (strings, total), 1) // FRESH_PLACES
    one, none = jnp.ones((), F32), jnp.zeros((), F32)
    start = jnp.dot(
        extents, jnp.where(string < owner, one, none).astype(BF16), preferred_element_type=F32
    )[:1]
    extent = jnp.dot(
        extents, jnp.where(string == owner, one, none).astype(BF16), preferred_element_type=F32
    )[:1]
    slot = (lax.broadcasted_iota(jnp.int32, (1, total), 1) % FRESH_PLACES).astype(F32)
    rank = jnp.where(slot < extent, start + slot, -1.0)
    row = lax.broadcasted_iota(jnp.int32, (count, total), 0).astype(F32)
    return jnp.where(rank == row, one, none).astype(BF16)


def place_rows(extent_ref, count, total):
    strings = extent_ref.shape[1]
    extents = extent_ref[...].astype(F32)
    string = lax.broadcasted_iota(jnp.int32, (total, strings), 1)
    owner = lax.broadcasted_iota(jnp.int32, (total, strings), 0) // FRESH_PLACES
    start = jnp.sum(jnp.where(string < owner, extents, 0.0), axis=1, keepdims=True)
    extent = jnp.sum(jnp.where(string == owner, extents, 0.0), axis=1, keepdims=True)
    slot = (lax.broadcasted_iota(jnp.int32, (total, 1), 0) % FRESH_PLACES).astype(F32)
    rank = jnp.where(slot < extent, start + slot, -1.0)
    row = lax.broadcasted_iota(jnp.int32, (total, count), 1).astype(F32)
    return jnp.where(rank == row, 1.0, 0.0).astype(BF16)


def attend_kernel(
    kv_size, tp_size, n_ref, extent_ref, w_ref, x_ref, resid_ref,
    ng, heads_part, landed, send_sems, recv_sems,
):
    place = Place(kv_size, tp_size)
    sizes = place.sizes
    z, y, x, c = (place.at[axis] for axis in ("z", "y", "x", "c"))
    steps = [(i, j) for i in range(sizes["x"]) for j in range(CORES) if i or j]
    across = [
        (place.partner("x", i), place.partner("c", j)) for i, j in steps
    ]
    greet(along(place, ("z", "y")) + [place.device(x=i, c=j) for i, j in across])
    sender = Sender(send_sems, recv_sems)
    half = n_ref.shape[0] // 2
    spans = [pl.ds(0, half), pl.ds(half, half)]
    in_z = [
        [
            sender.start(
                n_ref.at[span], ng.at[z, y, span], place.device(z=place.partner("z", step))
            )
            for step in range(1, sizes["z"])
        ]
        for span in spans
    ]
    ng[z, y] = n_ref[...]
    pick = pick_rows(extent_ref, resid_ref.shape[0], x_ref.shape[0])
    own = jnp.dot(pick, x_ref[...], preferred_element_type=F32)
    in_y = []
    for span, copies in zip(spans, in_z):
        for copy in copies:
            copy.wait_recv()
        in_y += [
            sender.start(
                ng.at[:, y, span], ng.at[:, y, span], place.device(y=place.partner("y", step))
            )
            for step in range(1, sizes["y"])
        ]
    for copy in in_y:
        copy.wait_recv()
    every = ng[...].reshape(pick.shape[1], n_ref.shape[1])
    chosen = jnp.dot(pick, every, preferred_element_type=F32).astype(BF16)
    product = jnp.dot(chosen, w_ref[...], preferred_element_type=F32).astype(BF16)
    block = x_ref.shape[1]
    for t in range(tp_size):
        heads_part[t] = product[:, t * block : (t + 1) * block]
    copies = [
        sender.start(heads_part.at[i * CORES + j], landed.at[n], place.device(x=i, c=j))
        for n, (i, j) in enumerate(across)
    ]
    total = heads_part[x * CORES + c].astype(F32)
    for n, copy in enumerate(copies):
        copy.wait_recv()
        total += landed[n].astype(F32)
    resid_ref[...] = (own + total).astype(BF16)
    sender.finish()


def mixer_kernel(
    kv_size, tp_size, x_ref, gain_ref, extent_ref, wg_hbm, wu_hbm, wd_hbm, out_ref,
    xg, gg, wg, wu, wd, own_part, core_part, core_recv, recvs, parts,
    send_sems, recv_sems, load_sems,
):
    place = Place(kv_size, tp_size)
    sizes = place.sizes
    at = place.at
    rows, block = x_ref.shape
    half = rows // 2
    features = kv_size * tp_size * block
    loads = [
        pltpu.make_async_copy(source, target, load_sems.at[n])
        for n, (source, target) in enumerate(((wg_hbm, wg), (wu_hbm, wu), (wd_hbm, wd)))
    ]
    for load in loads:
        load.start()
    greet(along(place, ("z", "y", "x", "c")))
    sender = Sender(send_sems, recv_sems)

    orders = (("z", "y", "x", "c"), ("z", "x", "y", "c"))

    def view(ref, done, span):
        lead = tuple(slice(None) if axis in done else at[axis] for axis in ("z", "y", "x"))
        if "c" in done:
            return ref.at[lead + (span, slice(None))]
        return ref.at[lead + (span, pl.ds(pl.multiple_of(at["c"] * block, block), block))]

    spans = [pl.ds(0, half), pl.ds(half, half)]

    def push(h, level):
        axis, done = orders[h][level], orders[h][:level]
        started = []
        for step in range(1, sizes[axis]):
            device = place.device(**{axis: place.partner(axis, step)})
            target = view(xg, done, spans[h])
            source = x_ref.at[spans[h]] if level == 0 else target
            started.append(sender.start(source, target, device))
            if h == 0:
                target = view(gg, done, slice(None))
                started.append(sender.start(gain_ref if level == 0 else target, target, device))
        return started

    flying = [push(0, 0), push(1, 0)]
    mine = pl.ds(pl.multiple_of(at["c"] * block, block), block)
    xg[at["z"], at["y"], at["x"], :, mine] = x_ref[...]
    gg[at["z"], at["y"], at["x"], :, mine] = gain_ref[...]
    spread = place_rows(extent_ref, rows, out_ref.shape[0])
    for level in range(1, 5):
        for h in range(2):
            for copy in flying[h]:
                copy.wait_recv()
            if level < 4:
                flying[h] = push(h, level)
    for load in loads:
        load.wait()

    units = [
        (i, j, k)
        for i in range(sizes["z"])
        for j in range(sizes["y"])
        for k in range(sizes["x"])
    ]
    wide = CORES * block
    hidden_units = wg.shape[0]
    gated = jnp.zeros((rows, hidden_units), F32)
    upward = jnp.zeros((rows, hidden_units), F32)
    squares = jnp.zeros((rows, wide), F32)

    def across(left, right):
        return lax.dot_general(
            left, right, (((1,), (1,)), ((), ())), preferred_element_type=F32
        )

    for n, unit in enumerate(units):
        value = xg[unit].astype(F32)
        squares += value * value
        piece = (value * gg[unit][:1]).astype(BF16)
        gated += across(piece, wg[:, n * wide : (n + 1) * wide])
        upward += across(piece, wu[:, n * wide : (n + 1) * wide])
    scale = lax.rsqrt(jnp.sum(squares, axis=1, keepdims=True) / features + epsilon)
    gated, upward = gated * scale, upward * scale
    hidden = (gated * jax.nn.sigmoid(gated) * upward).astype(BF16)

    copies = []
    for n, unit in enumerate(units):
        product = jnp.dot(hidden, wd[:, n * wide : (n + 1) * wide], preferred_element_type=F32)
        low, high = product[:, :block], product[:, block:]
        first = at["c"] == 0
        own_part[unit] = jnp.where(first, low, high)
        core_part[unit] = jnp.where(first, high, low).astype(BF16)
        if unit[1:] == (sizes["y"] - 1, sizes["x"] - 1):
            copies.append(
                sender.start(
                    core_part.at[unit[0]], core_recv.at[unit[0]],
                    place.device(c=place.partner("c", 1)),
                )
            )
    for copy in copies:
        copy.wait_recv()
    sums = (("x", "y", "z"), ("y", "x", "z"))
    axes = ("z", "y", "x")

    def index(h, done, moved=None):
        picked = []
        for axis in axes:
            if moved is not None and axis == moved[0]:
                picked.append(moved[1])
            elif axis in done:
                picked.append(at[axis])
            else:
                picked.append(slice(None))
        return tuple(picked)

    def add_core(h):
        span = slice(h * half, (h + 1) * half)
        return own_part[:, :, :, span] + core_recv[:, :, :, span].astype(F32)

    def send(h, level):
        axis, done = sums[h][level], sums[h][:level]
        source = parts[h][level]
        keep = [a for a in axes if a not in done]
        started = []
        for step in range(1, sizes[axis]):
            other = place.partner(axis, step)
            where = tuple(other if a == axis else slice(None) for a in keep)
            started.append(
                sender.start(
                    source.at[where] if where else source,
                    recvs[h][level].at[step - 1],
                    place.device(**{axis: other}),
                )
            )
        return started

    def reduce(h, level, copies):
        axis, done = sums[h][level], sums[h][:level]
        keep = [a for a in axes if a not in done]
        where = tuple(at[a] if a == axis else slice(None) for a in keep)
        for copy in copies:
            copy.wait_recv()
        total = parts[h][level][where].astype(F32)
        for step in range(1, sizes[axis]):
            total += recvs[h][level][step - 1].astype(F32)
        return total

    flying = []
    for h in range(2):
        parts[h][0][...] = add_core(h).astype(BF16)
        flying.append(send(h, 0))
    for level in range(2):
        for h in range(2):
            parts[h][level + 1][...] = reduce(h, level, flying[h]).astype(BF16)
            flying[h] = send(h, level + 1)
    down = jnp.concatenate([reduce(h, 2, flying[h]) for h in range(2)], axis=0)
    mixed = (x_ref[...].astype(F32) + down).astype(BF16)
    out_ref[...] = jnp.dot(spread, mixed, preferred_element_type=F32).astype(BF16)
    sender.finish()


def remote(kernel, out_shape, specs, scratch, name, identity):
    return pl.pallas_call(
        kernel,
        out_shape=out_shape,
        in_specs=specs,
        out_specs=jax.tree.map(lambda _: VM, out_shape),
        scratch_shapes=scratch,
        compiler_params=pltpu.CompilerParams(
            collective_id=identity, has_side_effects=True, vmem_limit_bytes=LIMIT
        ),
        name=name,
    )


def local(
    kv_size,
    tp_size,
    residual_entries,
    fresh_extents,
    memory_matrix,
    initial_rescale_vector,
    probe_matrix,
    retain_matrix,
    content_matrix,
    result_switch_matrix,
    retain_lower_limit,
    extra_shrink_log,
    lane_result_rescale,
    result_matrix,
    later_rescale_vector,
    mixer_switch_matrix,
    widening_matrix,
    narrowing_matrix,
):
    sequences, heads, head, _ = memory_matrix.shape
    own_rows = sequences * FRESH_PLACES
    all_rows, block = residual_entries.shape
    live_count = all_rows // 2
    width = probe_matrix.shape[1]
    features = block * kv_size * tp_size
    nz = 4 if kv_size % 4 == 0 else kv_size
    ny, nx = kv_size // nz, tp_size // CORES
    dma = pltpu.SemaphoreType.DMA

    piece = 4 * width // PIECES
    count = (nx - 1) + 1 + (PIECES + 1) * (ny - 1 + nz - 1)
    projected, squares = remote(
        functools.partial(project_kernel, kv_size, tp_size),
        (
            jax.ShapeDtypeStruct((4, own_rows, width), F32),
            jax.ShapeDtypeStruct((own_rows, block), F32),
        ),
        [VM] * 6,
        [
            pltpu.VMEM((nx, CORES, all_rows, block), BF16),
            pltpu.VMEM((all_rows, tp_size * block), BF16),
            pltpu.VMEM((PIECES, nz, ny, own_rows, piece), BF16),
            pltpu.VMEM((PIECES, max(ny - 1, 1), nz, own_rows, piece), BF16),
            pltpu.VMEM((PIECES, nz, own_rows, piece), BF16),
            pltpu.VMEM((PIECES, max(nz - 1, 1), own_rows, piece), BF16),
            pltpu.VMEM((nz, ny, own_rows, block), BF16),
            pltpu.VMEM((max(ny - 1, 1), nz, own_rows, block), BF16),
            pltpu.VMEM((nz, own_rows, block), BF16),
            pltpu.VMEM((max(nz - 1, 1), own_rows, block), BF16),
            dma((count,)),
            dma((count,)),
        ],
        "project",
        1,
    )(
        residual_entries,
        initial_rescale_vector.reshape(1, -1),
        probe_matrix,
        retain_matrix,
        content_matrix,
        result_switch_matrix,
    )

    extents = fresh_extents.reshape(1, -1)
    normed, new_state, gain_rows = pl.pallas_call(
        functools.partial(recur_kernel, features),
        out_shape=(
            jax.ShapeDtypeStruct((own_rows, width), BF16),
            jax.ShapeDtypeStruct(memory_matrix.shape, F32),
            jax.ShapeDtypeStruct((8, block), F32),
        ),
        in_specs=[VM] * 8,
        out_specs=(VM, VM, VM),
        compiler_params=pltpu.CompilerParams(vmem_limit_bytes=LIMIT),
        name="recur",
    )(
        projected,
        squares,
        memory_matrix,
        retain_lower_limit.reshape(1, -1),
        extra_shrink_log,
        extents,
        lane_result_rescale.reshape(1, -1),
        later_rescale_vector.reshape(1, -1),
    )

    count = 2 * (nz - 1) + 2 * (ny - 1) + (tp_size - 1)
    residual = remote(
        functools.partial(attend_kernel, kv_size, tp_size),
        jax.ShapeDtypeStruct((live_count, block), BF16),
        [VM] * 4,
        [
            pltpu.VMEM((nz, ny, own_rows, width), BF16),
            pltpu.VMEM((tp_size, live_count, block), BF16),
            pltpu.VMEM((tp_size - 1, live_count, block), BF16),
            dma((count,)),
            dma((count,)),
        ],
        "attend",
        2,
    )(normed, extents, result_matrix, residual_entries)

    half = live_count // 2
    sizes = {"z": nz, "y": ny, "x": nx}

    def buffers(order):
        left, landing, kept = ["z", "y", "x"], [], []
        for axis in order:
            kept.append(pltpu.VMEM(tuple(sizes[a] for a in left) + (half, block), BF16))
            left = [a for a in left if a != axis]
            landing.append(
                pltpu.VMEM(
                    (max(sizes[axis] - 1, 1),) + tuple(sizes[a] for a in left) + (half, block),
                    BF16,
                )
            )
        return kept, landing

    first, second = buffers(("x", "y", "z")), buffers(("y", "x", "z"))
    hops = nz + ny + nx - 3
    count = 3 * (hops + 1) + nz + 2 * hops
    hidden_units = mixer_switch_matrix.shape[1]
    mixed = remote(
        functools.partial(mixer_kernel, kv_size, tp_size),
        jax.ShapeDtypeStruct((all_rows, block), BF16),
        [VM, VM, VM, HBM, HBM, HBM],
        [
            pltpu.VMEM((nz, ny, nx, live_count, CORES * block), BF16),
            pltpu.VMEM((nz, ny, nx, 8, CORES * block), F32),
            pltpu.VMEM((hidden_units, features), BF16),
            pltpu.VMEM((hidden_units, features), BF16),
            pltpu.VMEM((hidden_units, features), BF16),
            pltpu.VMEM((nz, ny, nx, live_count, block), F32),
            pltpu.VMEM((nz, ny, nx, live_count, block), BF16),
            pltpu.VMEM((nz, ny, nx, live_count, block), BF16),
            [first[1], second[1]],
            [first[0], second[0]],
            dma((count,)),
            dma((count,)),
            dma((3,)),
        ],
        "mixer",
        3,
    )(
        residual,
        gain_rows,
        extents,
        mixer_switch_matrix.T,
        widening_matrix.T,
        narrowing_matrix,
    )
    return (mixed, new_state)


def plain_local(
    residual_entries,
    fresh_extents,
    memory_matrix,
    initial_rescale_vector,
    probe_matrix,
    retain_matrix,
    content_matrix,
    result_switch_matrix,
    retain_lower_limit,
    extra_shrink_log,
    lane_result_rescale,
    result_matrix,
    later_rescale_vector,
    mixer_switch_matrix,
    widening_matrix,
    narrowing_matrix,
):
    sequences_per_device = memory_matrix.shape[0]
    heads_per_device = memory_matrix.shape[1]
    rows_dev = sequences_per_device * FRESH_PLACES
    all_rows = residual_entries.shape[0]
    features = initial_rescale_vector.shape[0] * lax.axis_size("kv")
    kv_index = lax.axis_index("kv")
    tokens_wide = residual_entries.astype(jnp.float32)
    columns = lax.all_gather(residual_entries, "tp", axis=1, tiled=True)
    squares = lax.psum(jnp.sum(tokens_wide * tokens_wide, axis=1), ("kv", "tp"))
    own_squares = lax.dynamic_slice_in_dim(squares, kv_index * rows_dev, rows_dev)
    first_scale = lax.rsqrt(own_squares / features + epsilon)
    scaled = (columns.astype(jnp.float32) * initial_rescale_vector).astype(jnp.bfloat16)
    projected = (
        lax.psum_scatter(
            jnp.concatenate(
                [
                    jnp.dot(scaled, weight, preferred_element_type=jnp.float32)
                    for weight in (
                        probe_matrix,
                        retain_matrix,
                        content_matrix,
                        result_switch_matrix,
                    )
                ],
                axis=1,
            ).astype(jnp.bfloat16),
            "kv",
            scatter_dimension=0,
            tiled=True,
        ).astype(jnp.float32)
        * first_scale[:, None]
    )
    width_dev = probe_matrix.shape[1]
    shape_four = (sequences_per_device, FRESH_PLACES, heads_per_device, memory_matrix.shape[2])
    z_query = projected[:, :width_dev]
    z_forget = projected[:, width_dev : 2 * width_dev].reshape(shape_four)
    z_input = projected[:, 2 * width_dev : 3 * width_dev].reshape(shape_four)
    z_outgate = projected[:, 3 * width_dev :]
    own_lengths = lax.dynamic_slice_in_dim(
        fresh_extents, kv_index * sequences_per_device, sequences_per_device
    )
    living = jnp.arange(FRESH_PLACES, dtype=jnp.int32)[None, :] < own_lengths[:, None]
    query = jax.nn.silu(z_query).reshape(shape_four)
    bounds = retain_lower_limit.reshape(heads_per_device, memory_matrix.shape[2])
    retain_factor = bounds + (1.0 - bounds) * jax.nn.sigmoid(z_forget)
    shrink_exponent = jnp.log(retain_factor) + extra_shrink_log.reshape(
        sequences_per_device, FRESH_PLACES, heads_per_device, 1
    )
    decays = jnp.where(living[:, :, None, None], jnp.exp(shrink_exponent), 1.0)
    key_gate = jnp.where(living[:, :, None, None], 1.0 - retain_factor, 0.0)
    carried = memory_matrix
    outputs = []
    for position in range(FRESH_PLACES):
        carried = (
            decays[:, position, :, :, None] * carried
            + key_gate[:, position, :, :, None] * z_input[:, position, :, None, :]
        )
        outputs.append(
            jnp.einsum(
                "bhd,bhdv->bhv", query[:, position], carried, precision=lax.Precision.HIGHEST
            )
        )
    heads_out = jnp.stack(outputs, axis=1)
    heads_out = (
        heads_out
        * lax.rsqrt(jnp.mean(heads_out * heads_out, axis=-1, keepdims=True) + epsilon)
        * lane_result_rescale
    )
    normed = jnp.where(
        living.reshape(rows_dev)[:, None],
        heads_out.reshape(rows_dev, width_dev) * jax.nn.silu(z_outgate),
        0.0,
    ).astype(jnp.bfloat16)
    head_partial = jnp.dot(
        lax.all_gather(normed, "kv", axis=0, tiled=True),
        result_matrix,
        preferred_element_type=jnp.float32,
    ).astype(jnp.bfloat16)
    attended = lax.psum_scatter(head_partial, "tp", scatter_dimension=1, tiled=True).astype(
        jnp.float32
    )
    residual = (tokens_wide + attended).astype(jnp.bfloat16)
    resid_wide = residual.astype(jnp.float32)
    resid_squares = lax.psum(jnp.sum(resid_wide * resid_wide, axis=1), ("kv", "tp"))
    second_in = (
        resid_wide * later_rescale_vector * lax.rsqrt(resid_squares / features + epsilon)[:, None]
    ).astype(jnp.bfloat16)
    live_rows = (
        jnp.arange(FRESH_PLACES, dtype=jnp.int32)[None, :] < fresh_extents[:, None]
    ).reshape(all_rows)
    live_order = jnp.argsort(1 - live_rows.astype(jnp.int32), stable=True)[: all_rows // 2]
    mixer_input = jnp.take(second_in, live_order, axis=0)
    piece = lax.all_gather(mixer_input, ("kv", "tp"), axis=1, tiled=True)
    gated = jnp.dot(piece, mixer_switch_matrix, preferred_element_type=jnp.float32)
    upward = jnp.dot(piece, widening_matrix, preferred_element_type=jnp.float32)
    hidden = (jax.nn.silu(gated) * upward).astype(jnp.bfloat16)
    mixer_terms = lax.psum_scatter(
        jnp.dot(hidden, narrowing_matrix, preferred_element_type=jnp.float32),
        ("kv", "tp"),
        scatter_dimension=1,
        tiled=True,
    )
    down_terms = (
        jnp.zeros((all_rows, mixer_terms.shape[1]), jnp.float32).at[live_order].set(mixer_terms)
    )
    mixed = jnp.where(live_rows[:, None], resid_wide + down_terms, 0.0).astype(jnp.bfloat16)
    return (mixed, carried)


def solution(mesh):
    placed = (
        P(None, ("kv", "tp")),
        P(),
        P("kv", "tp", None, None),
        P("kv"),
        P("kv", "tp"),
        P("kv", "tp"),
        P("kv", "tp"),
        P("kv", "tp"),
        P("tp"),
        P("kv", "tp"),
        P(),
        P("tp", "kv"),
        P(("kv", "tp")),
        P(None, ("kv", "tp")),
        P(None, ("kv", "tp")),
        P(("kv", "tp"), None),
    )

    def step(residual_entries, *others):
        sizes = mesh.shape["kv"], mesh.shape["tp"]
        if residual_entries.shape[1] % 128:
            return plain_local(residual_entries, *others)
        return local(*sizes, residual_entries, *others)

    return jax.shard_map(
        step,
        mesh=mesh,
        in_specs=placed,
        out_specs=(P(None, ("kv", "tp")), P("kv", "tp", None, None)),
        check_vma=False,
    )
```
